32 devices in a mesh: tp: 8 (over z, x), dp: 4 (over y, core).
Axes of the slice: x: 2, y: 2, z: 4, core: 2. Of those that a mesh axis runs over, the one named last changes fastest.
Arguments:
- tokens: bfloat16 [128, 8, 4096], P('dp', None, 'tp'), may hold values from -12 to 12
- lengths: int32 [128], P('dp'), may hold values from 1 to 8, 384 in all
- norm_gains: float32 [2, 4096], replicated, may hold values from 0.1 to 1.9
- drive_proj: bfloat16 [2, 4096, 2048], P(None, 'dp', 'tp'), may hold values from -0.09375 to 0.09375
- open_proj: bfloat16 [2, 4096, 4096], P(None, 'dp', 'tp'), may hold values from -0.09375 to 0.09375
- glu_proj: bfloat16 [2, 2048, 2048], P(None, 'dp', 'tp'), may hold values from -0.125 to 0.125
- merge_proj: bfloat16 [2, 2048, 4096], P(None, 'dp', 'tp'), may hold values from -0.125 to 0.125
- exit_proj: bfloat16 [2, 4096, 4096], P(None, 'dp', 'tp'), may hold values from -0.09375 to 0.09375
- decay_rate: float32 [2, 128, 64], P(None, 'tp'), may hold values from 0.5 to 2
- turn_rate: float32 [2, 128, 64], P(None, 'tp'), may hold values from -3 to 3
- group_step_width: float32 [2, 128], P(None, 'tp'), may hold values from 0.005 to 0.3
- state_in: float32 [2, 2, 128, 64, 16], P(None, None, 'tp'), may hold values from -1 to 1
- state_out: float32 [2, 2, 128, 16, 64], P(None, None, 'tp'), may hold values from -0.5 to 0.5
- skip_gain: float32 [2, 2048], P(None, 'tp'), may hold values from -4 to 4
- carried_state: float32 [2, 2, 128, 8192], P(None, None, 'dp', 'tp'), may hold values from -6 to 6
Outputs:
- updated_tokens: bfloat16 [128, 8, 4096], P('dp', None, 'tp')
- new_state: float32 [2, 2, 128, 8192], P(None, None, 'dp', 'tp')
The draws below stay inside these ranges and needn't reach their ends.
Inputs may be any that keep to these rules, and one draw needn't show every extreme that they name: `lengths`: each sequence has at least one live slot, and some sequence has all 8.
All inputs are finite; a program needn't handle non-finite values. No bound on the sum of `lengths` on one device may be relied on, other than what follows from the above.
Results may differ from the reference program's by a relative error of at most 0.0055.
Values may be sent and summed in bfloat16 or wider, within the bound.
A program may use at most 128 MiB of HBM per device.

```python
import math
import jax
import jax.numpy as jnp
import numpy as np
from jax import lax

D = 4096
WIDTH = 2048
CHANNELS = 16
STATE = 64
STEPS = 8
LAYERS = 2
GROUPS = 128
BATCH = 128


def draw_tokens(key, part):
    first_key, second_key = jax.random.split(jax.random.fold_in(key, 11))
    block_count = 32
    blocks = jax.random.uniform(second_key, (BATCH, 1, block_count, 1), jnp.float32, math.log(0.3), math.log(3.0))
    factor = jnp.exp(blocks)
    values_drawn = jnp.clip(jax.random.normal(first_key, (BATCH, STEPS, block_count, D // block_count), jnp.float32), -4.0, 4.0)
    return (values_drawn * factor).reshape(BATCH, STEPS, D).astype(jnp.bfloat16)


def levels(key, shape, cuts, low, top_value):
    def one(dim, shards_of):
        heights = jax.random.uniform(jax.random.fold_in(jax.random.fold_in(key, 6), dim), (shards_of,), jnp.float32, low / len(cuts), top_value / len(cuts))
        return jnp.repeat(jnp.exp(heights), shape[dim] // shards_of).reshape((-1,) + (1,) * (len(shape) - dim - 1))

    gain = one(*cuts[0])
    for cut in cuts[1:]:
        gain = gain * one(*cut)
    return gain


def split_up(number_of, total, limit, slope):
    loads = [(1 << 20) // math.isqrt(grade ** slope) + 1 for grade in range(2, number_of + 1)]
    surplus, holding = total - limit - (number_of - 1), [1] * (number_of - 1)
    while surplus > 0:
        movable = [i for i in range(number_of - 1) if holding[i] < limit]
        pool, left = sum([loads[i] for i in movable]), surplus
        for i in movable:
            more = min(limit - holding[i], max(1, left * loads[i] // pool), surplus)
            holding[i] = holding[i] + more
            surplus = surplus - more
    return np.array([limit] + holding)


def uneven(stream_key, amount, total, reach, lean):
    if amount == 2:
        one = jax.random.randint(stream_key, (), max(1, total - reach), min(reach, total - 1) + 1)
        return jnp.stack([one, total - one])
    sizes = jnp.asarray(split_up(amount, total, reach, lean), jnp.int32)
    twos = (amount - 1) // 2
    donor, sink = sizes[1:1 + 2 * twos:2], sizes[2:2 + 2 * twos:2]
    room = jnp.minimum(donor - 1, reach - sink)
    passed = jax.random.randint(jax.random.fold_in(stream_key, 1), (twos,), 0, 1 << 20) % (room + 1)
    sizes = sizes.at[1:1 + 2 * twos:2].set(donor - passed).at[2:2 + 2 * twos:2].set(sink + passed)
    return sizes[jax.random.permutation(jax.random.fold_in(stream_key, 2), amount)]


def gaussian(stream_key, extent, scale, limit, cuts=(), dtype=jnp.bfloat16):
    loudness = levels(stream_key, extent, cuts, -0.22, 0.18) if cuts else 1.0
    array = jax.random.normal(stream_key, extent, jnp.float32) * scale * loudness
    return jnp.minimum(jnp.maximum(array, -limit), limit).astype(dtype)


def setup_inputs(seed: int = 0) -> dict:
    splits = jax.random.split(jax.random.key(seed), 16)
    return {
        "tokens": draw_tokens(jax.random.fold_in(splits[15], 71), 0),
        "lengths": uneven(splits[1], BATCH, 3 * BATCH, STEPS, 2).astype(jnp.int32),
        "norm_gains": jnp.clip(1.0 + 0.18 * jax.random.normal(splits[2], (LAYERS, D), jnp.float32), 0.1, 1.9),
        "drive_proj": gaussian(splits[3], (LAYERS, D, WIDTH), D ** -0.5, 0.09375, ((1, 4), (2, 8))),
        "open_proj": gaussian(splits[4], (LAYERS, D, D), D ** -0.5, 0.09375, ((1, 4), (2, 8))),
        "glu_proj": gaussian(splits[5], (LAYERS, WIDTH, WIDTH), WIDTH ** -0.5, 0.125, ((1, 4), (2, 8))),
        "merge_proj": gaussian(splits[6], (LAYERS, WIDTH, D), WIDTH ** -0.5, 0.125, ((1, 4), (2, 8))),
        "exit_proj": gaussian(splits[7], (LAYERS, D, D), D ** -0.5, 0.09375, ((1, 4), (2, 8))),
        "decay_rate": jnp.clip(jnp.exp(math.log(2.0) - 1.3862944 * jax.random.uniform(splits[8], (LAYERS, GROUPS, STATE), jnp.float32) ** levels(splits[8], (LAYERS, GROUPS, STATE), ((1, 8),), -0.2, 0.2)), 0.5, 2.0),
        "turn_rate": jnp.clip(jax.random.uniform(splits[9], (LAYERS, GROUPS, STATE), jnp.float32, -3.0, 3.0) * levels(splits[9], (LAYERS, GROUPS, STATE), ((1, 8),), -0.4, 0.0), -3.0, 3.0),
        "group_step_width": jnp.clip(jnp.exp(math.log(0.3) - 4.0943446 * jax.random.uniform(splits[10], (LAYERS, GROUPS), jnp.float32) ** levels(splits[10], (LAYERS, GROUPS), ((1, 8),), -0.2, 0.2)), 0.005, 0.3),
        "state_in": gaussian(splits[11], (LAYERS, 2, GROUPS, STATE, CHANNELS), (2 * CHANNELS) ** -0.5, 1.0, ((2, 8),), jnp.float32),
        "state_out": gaussian(splits[12], (LAYERS, 2, GROUPS, CHANNELS, STATE), (2 * STATE) ** -0.5, 0.5, ((2, 8),), jnp.float32),
        "skip_gain": gaussian(splits[13], (LAYERS, WIDTH), 1.0, 4.0, ((1, 8),), jnp.float32),
        "carried_state": gaussian(splits[14], (LAYERS, 2, BATCH, GROUPS * STATE), 1.0, 6.0, ((2, 4), (3, 8)), jnp.float32),
    }


EPS = 1e-05

def state_update(drive, active, current_rate, turn_now, size_now, in_pair, output_couple, skip_now, carried):
    sequences, positions = active.shape
    groups, entries = current_rate.shape
    members = in_pair.shape[-1]
    real_eig = -current_rate
    step_len = size_now[:, None]
    magnitude = jnp.exp(step_len * real_eig)
    decay_real = magnitude * jnp.cos(step_len * turn_now)
    decay_imag = magnitude * jnp.sin(step_len * turn_now)
    divisor = real_eig * real_eig + turn_now * turn_now
    hold_real = ((decay_real - 1.0) * real_eig + decay_imag * turn_now) / divisor
    hold_imag = (decay_imag * real_eig - (decay_real - 1.0) * turn_now) / divisor
    inject_real = hold_real[..., None] * in_pair[0] - hold_imag[..., None] * in_pair[1]
    inject_imag = hold_real[..., None] * in_pair[1] + hold_imag[..., None] * in_pair[0]
    inputs = drive.reshape(sequences, positions, groups, members)
    pushed_real = jnp.einsum('gpc,bsgc->bsgp', inject_real, inputs, precision=lax.Precision.HIGHEST)
    pushed_imag = jnp.einsum('gpc,bsgc->bsgp', inject_imag, inputs, precision=lax.Precision.HIGHEST)
    state_real_part = carried[0].reshape(sequences, groups, entries)
    state_imaginary = carried[1].reshape(sequences, groups, entries)
    readings = []
    for position in range(positions):
        active_now = (active[:, position] > 0)[:, None, None]
        moved_real = decay_real * state_real_part - decay_imag * state_imaginary + pushed_real[:, position]
        moved_imag = decay_real * state_imaginary + decay_imag * state_real_part + pushed_imag[:, position]
        state_real_part = jnp.where(active_now, moved_real, state_real_part)
        state_imaginary = jnp.where(active_now, moved_imag, state_imaginary)
        readout_value = jnp.einsum('sal,usl->usa', output_couple[0], state_real_part, precision=lax.Precision.HIGHEST) - jnp.einsum('sal,usl->usa', output_couple[1], state_imaginary, precision=lax.Precision.HIGHEST)
        readings.append(readout_value)
    readout = jnp.stack(readings, axis=1) + skip_now.reshape(groups, members) * inputs
    final = jnp.stack([state_real_part.reshape(sequences, groups * entries), state_imaginary.reshape(sequences, groups * entries)])
    return (readout.reshape(sequences * positions, groups * members), final)

def reference(tokens, lengths, norm_gains, drive_proj, open_proj, glu_proj, merge_proj, exit_proj, decay_rate, turn_rate, group_step_width, state_in, state_out, skip_gain, carried_state):
    sequences, positions, model_width = tokens.shape
    row_count = sequences * positions
    active = (lax.broadcasted_iota(jnp.int32, (sequences, positions), 1) < lengths[:, None]).astype(jnp.int32)
    active_rows = active.reshape(row_count, 1).astype(jnp.float32)
    residual = tokens.reshape(row_count, model_width)
    states = []
    for layer_index in range(LAYERS):
        values = residual.astype(jnp.float32)
        inverse_rms = lax.rsqrt(lax.optimization_barrier(jnp.mean(values * values, axis=1, keepdims=True)) + EPS)
        normed = (values * inverse_rms * norm_gains[layer_index]).astype(jnp.bfloat16)
        drive = jnp.dot(normed, drive_proj[layer_index], preferred_element_type=jnp.float32)
        gate_open = jax.nn.sigmoid(jnp.dot(normed, open_proj[layer_index], preferred_element_type=jnp.float32))
        readout, final = state_update(drive, active, decay_rate[layer_index], turn_rate[layer_index], group_step_width[layer_index], state_in[layer_index], state_out[layer_index], skip_gain[layer_index], carried_state[layer_index])
        states.append(final)
        activated = jax.nn.gelu(readout).astype(jnp.bfloat16)
        gating = jnp.dot(activated, glu_proj[layer_index], preferred_element_type=jnp.float32)
        gated = (activated.astype(jnp.float32) * jax.nn.sigmoid(gating)).astype(jnp.bfloat16)
        merged = jnp.dot(gated, merge_proj[layer_index], preferred_element_type=jnp.float32)
        mixed = (gate_open * merged).astype(jnp.bfloat16)
        branch = jnp.dot(mixed, exit_proj[layer_index], preferred_element_type=jnp.float32)
        residual = (residual.astype(jnp.float32) + active_rows * branch).astype(jnp.bfloat16)
    return (residual.reshape(sequences, positions, model_width), jnp.stack(states))
```

```python
import functools
import jax
import jax.numpy as jnp
from jax import lax
from jax.experimental import pallas as pl
from jax.experimental.pallas import tpu as pltpu
from jax.sharding import PartitionSpec as P

EPS = 1e-05


def state_update(
    drive, active, current_rate, turn_now, size_now, in_pair, output_couple, skip_now, carried
):
    sequences, positions = active.shape
    groups, entries = current_rate.shape
    members = in_pair.shape[-1]
    real_eig = -current_rate
    step_len = size_now[:, None]
    magnitude = jnp.exp(step_len * real_eig)
    decay_real = magnitude * jnp.cos(step_len * turn_now)
    decay_imag = magnitude * jnp.sin(step_len * turn_now)
    divisor = real_eig * real_eig + turn_now * turn_now
    hold_real = ((decay_real - 1.0) * real_eig + decay_imag * turn_now) / divisor
    hold_imag = (decay_imag * real_eig - (decay_real - 1.0) * turn_now) / divisor
    inject_real = hold_real[..., None] * in_pair[0] - hold_imag[..., None] * in_pair[1]
    inject_imag = hold_real[..., None] * in_pair[1] + hold_imag[..., None] * in_pair[0]
    inputs = drive.reshape(sequences, positions, groups, members)
    pushed_real = jnp.einsum("gpc,bsgc->bsgp", inject_real, inputs, precision=lax.Precision.HIGHEST)
    pushed_imag = jnp.einsum("gpc,bsgc->bsgp", inject_imag, inputs, precision=lax.Precision.HIGHEST)
    state_real_part = carried[0].reshape(sequences, groups, entries)
    state_imaginary = carried[1].reshape(sequences, groups, entries)
    readings = []
    for position in range(positions):
        active_now = (active[:, position] > 0)[:, None, None]
        moved_real = (
            decay_real * state_real_part - decay_imag * state_imaginary + pushed_real[:, position]
        )
        moved_imag = (
            decay_real * state_imaginary + decay_imag * state_real_part + pushed_imag[:, position]
        )
        state_real_part = jnp.where(active_now, moved_real, state_real_part)
        state_imaginary = jnp.where(active_now, moved_imag, state_imaginary)
        readout_value = jnp.einsum(
            "sal,usl->usa", output_couple[0], state_real_part, precision=lax.Precision.HIGHEST
        ) - jnp.einsum(
            "sal,usl->usa", output_couple[1], state_imaginary, precision=lax.Precision.HIGHEST
        )
        readings.append(readout_value)
    readout = jnp.stack(readings, axis=1) + skip_now.reshape(groups, members) * inputs
    final = jnp.stack(
        [
            state_real_part.reshape(sequences, groups * entries),
            state_imaginary.reshape(sequences, groups * entries),
        ]
    )
    return (readout.reshape(sequences * positions, groups * members), final)


def widen_model(values):
    return lax.all_gather(values, "tp", axis=1, tiled=True)


def widen_branch(values):
    return lax.all_gather(values, "tp", axis=1, tiled=True)


def project(gathered, weight):
    return jnp.dot(
        gathered,
        lax.all_gather(weight, "dp", axis=0, tiled=True),
        preferred_element_type=jnp.float32,
    )


def shards(
    tokens,
    lengths,
    norm_gains,
    drive_proj,
    open_proj,
    glu_proj,
    merge_proj,
    exit_proj,
    decay_rate,
    turn_rate,
    group_step_width,
    state_in,
    state_out,
    skip_gain,
    carried_state,
):
    sequences, positions, local_width = tokens.shape
    row_count = sequences * positions
    model_width = local_width * lax.axis_size("tp")
    first_col = lax.axis_index("tp") * local_width
    active = (lax.broadcasted_iota(jnp.int32, (sequences, positions), 1) < lengths[:, None]).astype(
        jnp.int32
    )
    active_rows = active.reshape(row_count, 1).astype(jnp.float32)
    residual = tokens.reshape(row_count, local_width)
    states = []
    for layer_index in range(norm_gains.shape[0]):
        norm_gain = norm_gains[layer_index]
        own_values = residual.astype(jnp.float32)
        squared_sum = lax.psum(jnp.sum(own_values * own_values, axis=1), "tp")
        inverse_rms = lax.rsqrt(squared_sum / model_width + EPS)[:, None]
        own_gain = lax.dynamic_slice_in_dim(norm_gain, first_col, local_width, 0)
        gathered = widen_model((own_values * inverse_rms * own_gain).astype(jnp.bfloat16))
        drive = project(gathered, drive_proj[layer_index])
        gate_open = jax.nn.sigmoid(project(gathered, open_proj[layer_index]))
        readout, final = state_update(
            drive,
            active,
            decay_rate[layer_index],
            turn_rate[layer_index],
            group_step_width[layer_index],
            state_in[layer_index],
            state_out[layer_index],
            skip_gain[layer_index],
            carried_state[layer_index],
        )
        states.append(final)
        activated = jax.nn.gelu(readout).astype(jnp.bfloat16)
        gating = project(widen_branch(activated), glu_proj[layer_index])
        gated = (activated.astype(jnp.float32) * jax.nn.sigmoid(gating)).astype(jnp.bfloat16)
        merged = project(widen_branch(gated), merge_proj[layer_index])
        mixed = (gate_open * merged).astype(jnp.bfloat16)
        branch = project(widen_model(mixed), exit_proj[layer_index])
        residual = (residual.astype(jnp.float32) + active_rows * branch).astype(jnp.bfloat16)
    return (residual.reshape(sequences, positions, local_width), jnp.stack(states))


def fused_kernel(
    dims,
    tok, pack_own, unpack_own, keep, unpack, pack, gains, decay, inject, outmix, skip, carried,
    w_drive, w_open, w_glu, w_merge, w_exit,
    out_tok, out_state,
    v_drive, v_open, v_glu, v_merge, v_exit,
    row_send, row_recv, a_send, a_recv, c_send, c_recv,
    x_src, x_recv, y_src, y_recv, st_recv, st_new, nst_recv, fin_recv,
    inv_buf, gate_buf, act_buf,
    w_sem, row_ss, row_rs, a_ss, a_rs, c_ss, c_rs, x_ss, x_rs, y_ss, y_rs,
    st_ss, st_rs, n_ss, n_rs, f_ss, f_rs,
):
    layers, nd, nt, rows, model = dims
    ratio = nt // nd
    chunk = rows // nd
    half = rows // 2
    f32, bf16 = jnp.float32, jnp.bfloat16
    d = lax.axis_index("dp")
    t = lax.axis_index("tp")
    home = t // ratio
    place = lax.rem(t, ratio)
    batch_own = carried.shape[2]
    batch = batch_own * nd
    own_ch = inject.shape[2] // 2
    width = c_send.shape[-1] // 2
    steps = unpack.shape[0] // batch

    loads = []
    for i, (src, dst) in enumerate(
        ((w_drive, v_drive), (w_open, v_open), (w_glu, v_glu), (w_merge, v_merge), (w_exit, v_exit))
    ):
        for l in range(layers):
            copy = pltpu.make_async_copy(src.at[l], dst.at[l], w_sem.at[i, l])
            copy.start()
            loads.append(copy)

    def weight(i, l):
        loads[i * layers + l].wait()

    barrier = pltpu.get_barrier_semaphore()
    total = nd * nt
    flat = t * nd + d

    def greet(i, carry):
        other = lax.rem(flat + i, total)
        pl.semaphore_signal(
            barrier, inc=1,
            device_id={"tp": other // nd, "dp": lax.rem(other, nd)},
            device_id_type=pl.DeviceIdType.MESH,
        )
        return carry

    lax.fori_loop(1, total, greet, 0)
    pl.semaphore_wait(barrier, total - 1)

    pending = []

    def send(src, dst, ss, rs, to_dp, to_tp, is_self):
        far = pltpu.make_async_remote_copy(
            src_ref=src, dst_ref=dst, send_sem=ss, recv_sem=rs,
            device_id={"tp": to_tp, "dp": to_dp}, device_id_type=pl.DeviceIdType.MESH,
        )
        if is_self is None:
            far.start()
        else:
            @pl.when(is_self)
            def _():
                pltpu.make_async_copy(src, dst, rs).start()

            @pl.when(jnp.logical_not(is_self))
            def _():
                far.start()

        pending.append((far, is_self))

    def arrive(dst, rs):
        pltpu.make_async_copy(dst, dst, rs).wait()

    def send_row(k, c):
        send(row_send.at[k, c], row_recv.at[k, d], row_ss.at[k, c], row_rs.at[k, d], c, t, d == c)

    def row_sum(k):
        acc = None
        for s in range(nd):
            arrive(row_recv.at[k, s], row_rs.at[k, s])
            v = row_recv[k, s].astype(f32)
            acc = v if acc is None else acc + v
        return acc

    def spread_x(k):
        slot = place * nd + d
        for j in range(nt):
            to = lax.rem(t + j, nt)
            send(
                x_src.at[k], x_recv.at[k, place, pl.ds(d * chunk, chunk)],
                x_ss.at[k, j], x_rs.at[k, slot], home, to, (d == home) if j == 0 else None,
            )

    def take_x(k):
        for p in range(ratio):
            for s in range(nd):
                arrive(x_recv.at[k, p, pl.ds(s * chunk, chunk)], x_rs.at[k, p * nd + s])

    def spread_y(k):
        slot = place * nd + d
        for j in range(nt):
            to = lax.rem(t + j, nt)
            send(
                y_src.at[k], y_recv.at[k, slot],
                y_ss.at[k, j], y_rs.at[k, slot], home, to, (d == home) if j == 0 else None,
            )

    def take_y(k):
        parts = []
        for p in range(ratio):
            for s in range(nd):
                arrive(y_recv.at[k, p * nd + s], y_rs.at[k, p * nd + s])
                v = y_recv[k, p * nd + s]
                parts.append(jnp.concatenate([v[:, :width], v[:, width:]], axis=0))
        return jnp.concatenate(parts, axis=1)

    def fold(v):
        return jnp.concatenate([v[:half], v[half:]], axis=1)

    for c in range(nd):
        part = jnp.dot(pack_own[c * chunk:(c + 1) * chunk, :], tok[...], preferred_element_type=f32)
        row_send[0, c] = part.astype(bf16)
        send_row(0, c)
    for c in range(nd):
        send(
            carried.at[:, :, :, pl.ds(c * own_ch, own_ch)], st_recv.at[d],
            st_ss.at[c], st_rs.at[d], c, t, d == c,
        )
    residual = row_sum(0).astype(bf16)
    cols = tok.shape[1]
    for l in range(layers):
        x_src[2 * l] = residual
        spread_x(2 * l)
        if l == 0:
            for s in range(nd):
                arrive(st_recv.at[s], st_rs.at[s])
        take_x(2 * l)
        scaled, squares = [], None
        for p in range(ratio):
            raw = x_recv[2 * l, p].astype(f32)
            sq = jnp.sum(raw * raw, axis=1, keepdims=True)
            squares = sq if squares is None else squares + sq
            scaled.append((raw * gains[l, p]).astype(bf16))
        normed = jnp.concatenate(scaled, axis=1)
        weight(0, l)
        drive = jnp.dot(normed, v_drive[l], preferred_element_type=f32)
        high = squares.astype(bf16)
        low = (squares - high.astype(f32)).astype(bf16)
        lane = lax.broadcasted_iota(jnp.int32, (rows, width), 1)
        tail = jnp.where(
            lane == 0, high.astype(f32), jnp.where(lane == 1, low.astype(f32), 0.0)
        ).astype(bf16)
        for c in range(nd):
            a_send[l, c] = jnp.concatenate(
                [drive[:, c * width:(c + 1) * width].astype(bf16), tail], axis=1
            )
            send(a_send.at[l, c], a_recv.at[l, d], a_ss.at[l, c], a_rs.at[l, d], c, t, d == c)
        weight(1, l)
        k_open = 1 + 3 * l
        for c in range(nd):
            part = jnp.dot(
                normed[c * chunk:(c + 1) * chunk], v_open[l], preferred_element_type=f32
            )
            row_send[k_open, c] = part.astype(bf16)
            send_row(k_open, c)
        summed = None
        for s in range(nd):
            arrive(a_recv.at[l, s], a_rs.at[l, s])
            v = a_recv[l, s].astype(f32)
            summed = v if summed is None else summed + v
        full_sq = summed[:, width:width + 1] + summed[:, width + 1:width + 2]
        inverse = lax.rsqrt(full_sq / model + EPS)
        inv_buf[...] = jnp.broadcast_to(inverse, inv_buf.shape)
        lane2 = lax.broadcasted_iota(jnp.int32, summed.shape, 1)
        feed = jnp.where(lane2 < width, summed * inverse, jnp.where(lane2 == width, 1.0, 0.0))
        feed = feed.astype(bf16)
        real = jnp.concatenate([st_recv[s, l, 0] for s in range(nd)], axis=0)
        imag = jnp.concatenate([st_recv[s, l, 1] for s in range(nd)], axis=0)
        dr, di = decay[l, 0], decay[l, 1]
        for step in range(steps):
            span = slice(step * batch, (step + 1) * batch)
            u = jnp.dot(unpack[span, :], feed, preferred_element_type=f32)
            live = u[:, width:width + 1] > 0.5
            push = jnp.dot(u.astype(bf16), inject[l], preferred_element_type=f32)
            moved_real = dr * real - di * imag + push[:, :own_ch]
            moved_imag = dr * imag + di * real + push[:, own_ch:]
            real = jnp.where(live, moved_real, real)
            imag = jnp.where(live, moved_imag, imag)
            both = jnp.concatenate([real, imag], axis=1).astype(bf16)
            read = jnp.dot(both, outmix[l], preferred_element_type=f32) + skip[l] * u
            act_buf[span, :] = jax.nn.gelu(read).astype(bf16)
        st_new[l, 0] = real
        st_new[l, 1] = imag
        packed = jnp.dot(pack[...], act_buf[...], preferred_element_type=f32).astype(bf16)
        activated = fold(packed[:, :width])
        y_src[2 * l] = activated
        spread_y(2 * l)
        for c in range(nd):
            send(
                st_new.at[l, :, pl.ds(c * batch_own, batch_own)], nst_recv.at[d, l],
                n_ss.at[l, c], n_rs.at[l, d], c, t, d == c,
            )
        mine = pl.ds(pl.multiple_of(d * chunk, chunk), chunk)
        gate_buf[...] = jax.nn.sigmoid(row_sum(k_open) * inv_buf[mine, 0:1])
        wide = take_y(2 * l)
        weight(2, l)
        gating = jnp.dot(wide, v_glu[l], preferred_element_type=f32).astype(bf16)
        for c in range(nd):
            c_send[l, c] = fold(gating[:, c * width:(c + 1) * width])
            send(c_send.at[l, c], c_recv.at[l, d], c_ss.at[l, c], c_rs.at[l, d], c, t, d == c)
        summed = None
        for s in range(nd):
            arrive(c_recv.at[l, s], c_rs.at[l, s])
            v = c_recv[l, s].astype(f32)
            summed = v if summed is None else summed + v
        y_src[2 * l + 1] = (activated.astype(f32) * jax.nn.sigmoid(summed)).astype(bf16)
        spread_y(2 * l + 1)
        wide = take_y(2 * l + 1)
        weight(3, l)
        for c in range(nd):
            part = jnp.dot(wide[c * chunk:(c + 1) * chunk], v_merge[l], preferred_element_type=f32)
            row_send[k_open + 1, c] = part.astype(bf16)
            send_row(k_open + 1, c)
        x_src[2 * l + 1] = (gate_buf[...] * row_sum(k_open + 1)).astype(bf16)
        spread_x(2 * l + 1)
        take_x(2 * l + 1)
        weight(4, l)
        for c in range(nd):
            part = None
            for p in range(ratio):
                v = jnp.dot(
                    x_recv[2 * l + 1, p, c * chunk:(c + 1) * chunk],
                    v_exit[l, p * cols:(p + 1) * cols],
                    preferred_element_type=f32,
                )
                part = v if part is None else part + v
            row_send[k_open + 2, c] = part.astype(bf16)
            send_row(k_open + 2, c)
        residual = (residual.astype(f32) + row_sum(k_open + 2)).astype(bf16)
    x_src[2 * layers] = residual
    for c in range(nd):
        send(
            x_src.at[2 * layers], fin_recv.at[pl.ds(d * chunk, chunk)],
            f_ss.at[c], f_rs.at[d], c, t, d == c,
        )
    for l in range(layers):
        for s in range(nd):
            arrive(nst_recv.at[s, l], n_rs.at[l, s])
            for part in range(2):
                out_state[l, part, :, s * own_ch:(s + 1) * own_ch] = nst_recv[s, l, part]
    for s in range(nd):
        arrive(fin_recv.at[pl.ds(s * chunk, chunk)], f_rs.at[s])
    spread = jnp.dot(unpack_own[...], fin_recv[...], preferred_element_type=f32)
    out_tok[...] = jnp.where(keep[...] > 0.5, spread, tok[...].astype(f32)).astype(bf16)
    for far, is_self in pending:
        if is_self is None:
            far.wait_send()
        else:
            pl.when(jnp.logical_not(is_self))(far.wait_send)


def fused_shards(
    tokens, lengths, norm_gains, drive_proj, open_proj, glu_proj, merge_proj, exit_proj,
    decay_rate, turn_rate, group_step_width, state_in, state_out, skip_gain, carried_state,
):
    f32, bf16 = jnp.float32, jnp.bfloat16
    nd, nt = lax.axis_size("dp"), lax.axis_size("tp")
    d, t = lax.axis_index("dp"), lax.axis_index("tp")
    layers = norm_gains.shape[0]
    own, steps, cols = tokens.shape
    batch = own * nd
    rows = 3 * batch
    model = cols * nt
    ratio = nt // nd
    groups_own = decay_rate.shape[1]
    few = groups_own // nd
    entries = decay_rate.shape[2]
    members = state_in.shape[-1]
    width = few * members
    own_ch = few * entries
    chunk = rows // nd

    everyone = lax.all_gather(lengths, "dp", axis=0, tiled=True)
    starts = jnp.cumsum(everyone) - everyone
    slot = jnp.arange(steps, dtype=jnp.int32)
    where_tb = jnp.where(
        slot[:, None] < everyone[None, :], starts[None, :] + slot[:, None], -1
    ).reshape(steps * batch)
    own_starts = lax.dynamic_slice_in_dim(starts, d * own, own, 0)
    where_own = jnp.where(
        slot[None, :] < lengths[:, None], own_starts[:, None] + slot[None, :], -1
    ).reshape(own * steps)
    index = jnp.arange(rows, dtype=jnp.int32)
    unpack = (where_tb[:, None] == index[None, :]).astype(bf16)
    pack = (index[:, None] == where_tb[None, :]).astype(bf16)
    unpack_own = (where_own[:, None] == index[None, :]).astype(bf16)
    pack_own = (index[:, None] == where_own[None, :]).astype(bf16)
    keep = (where_own >= 0).astype(f32)[:, None]
    gains = lax.dynamic_slice_in_dim(norm_gains, d * (model // nd), model // nd, 1).reshape(
        layers, ratio, 1, cols
    )

    def mine(v, axis):
        return lax.dynamic_slice_in_dim(v, d * few, few, axis)

    real_eig = -mine(decay_rate, 1)
    turn_now = mine(turn_rate, 1)
    step_len = mine(group_step_width, 1)[..., None]
    in_pair, out_pair = mine(state_in, 2), mine(state_out, 2)
    skip_now = mine(skip_gain.reshape(layers, groups_own, members), 1).reshape(layers, 1, width)
    magnitude = jnp.exp(step_len * real_eig)
    decay_real = magnitude * jnp.cos(step_len * turn_now)
    decay_imag = magnitude * jnp.sin(step_len * turn_now)
    divisor = real_eig * real_eig + turn_now * turn_now
    hold_real = ((decay_real - 1.0) * real_eig + decay_imag * turn_now) / divisor
    hold_imag = (decay_imag * real_eig - (decay_real - 1.0) * turn_now) / divisor
    inject_real = hold_real[..., None] * in_pair[:, 0] - hold_imag[..., None] * in_pair[:, 1]
    inject_imag = hold_real[..., None] * in_pair[:, 1] + hold_imag[..., None] * in_pair[:, 0]
    eye = jnp.eye(few, dtype=f32)
    both = jnp.stack([inject_real, inject_imag], axis=1)
    inject = (
        jnp.transpose(both, (0, 2, 4, 1, 3))[:, :, :, :, None, :]
        * eye[None, :, None, None, :, None]
    ).reshape(layers, width, 2 * own_ch)
    inject = jnp.pad(inject, ((0, 0), (0, width), (0, 0))).astype(bf16)
    signed = jnp.stack([out_pair[:, 0], -out_pair[:, 1]], axis=1)
    outmix = (
        jnp.transpose(signed, (0, 1, 2, 4, 3))[:, :, :, :, None, :]
        * eye[None, None, :, None, :, None]
    ).reshape(layers, 2 * own_ch, width)
    outmix = jnp.pad(outmix, ((0, 0), (0, 0), (0, width))).astype(bf16)
    skip = jnp.pad(skip_now, ((0, 0), (0, 0), (0, width)))
    decay = jnp.stack([decay_real, decay_imag], axis=1).reshape(layers, 2, 1, own_ch)

    n_row = 1 + 3 * layers
    half = rows // 2
    vm = pltpu.VMEM
    dma = pltpu.SemaphoreType.DMA
    weights = (drive_proj, open_proj, glu_proj, merge_proj, exit_proj)
    scratch = [vm(w.shape, bf16) for w in weights] + [
        vm((n_row, nd, chunk, cols), bf16),
        vm((n_row, nd, chunk, cols), bf16),
        vm((layers, nd, rows, 2 * width), bf16),
        vm((layers, nd, rows, 2 * width), bf16),
        vm((layers, nd, half, 2 * width), bf16),
        vm((layers, nd, half, 2 * width), bf16),
        vm((2 * layers + 1, chunk, cols), bf16),
        vm((2 * layers, ratio, rows, cols), bf16),
        vm((2 * layers, half, 2 * width), bf16),
        vm((2 * layers, nt, half, 2 * width), bf16),
        vm((nd, layers, 2, own, own_ch), f32),
        vm((layers, 2, batch, own_ch), f32),
        vm((nd, layers, 2, own, own_ch), f32),
        vm((rows, cols), bf16),
        vm((rows, 128), f32),
        vm((chunk, cols), f32),
        vm((steps * batch, 2 * width), bf16),
        dma((5, layers)),
        dma((n_row, nd)), dma((n_row, nd)),
        dma((layers, nd)), dma((layers, nd)),
        dma((layers, nd)), dma((layers, nd)),
        dma((2 * layers, nt)), dma((2 * layers, nt)),
        dma((2 * layers, nt)), dma((2 * layers, nt)),
        dma((nd,)), dma((nd,)),
        dma((layers, nd)), dma((layers, nd)),
        dma((nd,)), dma((nd,)),
    ]
    inside = pl.BlockSpec(memory_space=pltpu.VMEM)
    outside = pl.BlockSpec(memory_space=pl.ANY)
    out_rows, out_state = pl.pallas_call(
        functools.partial(fused_kernel, (layers, nd, nt, rows, model)),
        out_shape=(
            jax.ShapeDtypeStruct((own * steps, cols), bf16),
            jax.ShapeDtypeStruct(carried_state.shape, f32),
        ),
        in_specs=[inside] * 12 + [outside] * 5,
        out_specs=(inside, inside),
        scratch_shapes=scratch,
        compiler_params=pltpu.CompilerParams(
            collective_id=0, has_side_effects=True, vmem_limit_bytes=60 * 1024 * 1024
        ),
    )(
        tokens.reshape(own * steps, cols), pack_own, unpack_own, keep, unpack, pack,
        gains, decay, inject, outmix, skip, carried_state, *weights,
    )
    return out_rows.reshape(own, steps, cols), out_state


def solution(mesh):
    in_specs = (
        P("dp", None, "tp"),
        P("dp"),
        P(),
        P(None, "dp", "tp"),
        P(None, "dp", "tp"),
        P(None, "dp", "tp"),
        P(None, "dp", "tp"),
        P(None, "dp", "tp"),
        P(None, "tp", None),
        P(None, "tp", None),
        P(None, "tp"),
        P(None, None, "tp", None, None),
        P(None, None, "tp", None, None),
        P(None, "tp"),
        P(None, None, "dp", "tp"),
    )
    out_specs = (P("dp", None, "tp"), P(None, None, "dp", "tp"))
    ways, nd = mesh.shape["tp"], mesh.shape["dp"]

    def run(*args):
        groups = args[8].shape[1] // ways
        whole_groups = groups % nd == 0 and ways % nd == 0
        body = fused_shards if whole_groups else shards
        return jax.shard_map(body, mesh=mesh, in_specs=in_specs, out_specs=out_specs, check_vma=False)(*args)

    return run
```

```python
import functools
import jax
import jax.numpy as jnp
from jax import lax
from jax.experimental import pallas as pl
from jax.experimental.pallas import tpu as pltpu
from jax.sharding import PartitionSpec as P

EPS = 1e-05


def state_update(
    drive, active, current_rate, turn_now, size_now, in_pair, output_couple, skip_now, carried
):
    sequences, positions = active.shape
    groups, entries = current_rate.shape
    members = in_pair.shape[-1]
    real_eig = -current_rate
    step_len = size_now[:, None]
    magnitude = jnp.exp(step_len * real_eig)
    decay_real = magnitude * jnp.cos(step_len * turn_now)
    decay_imag = magnitude * jnp.sin(step_len * turn_now)
    divisor = real_eig * real_eig + turn_now * turn_now
    hold_real = ((decay_real - 1.0) * real_eig + decay_imag * turn_now) / divisor
    hold_imag = (decay_imag * real_eig - (decay_real - 1.0) * turn_now) / divisor
    inject_real = hold_real[..., None] * in_pair[0] - hold_imag[..., None] * in_pair[1]
    inject_imag = hold_real[..., None] * in_pair[1] + hold_imag[..., None] * in_pair[0]
    inputs = drive.reshape(sequences, positions, groups, members)
    pushed_real = jnp.einsum("gpc,bsgc->bsgp", inject_real, inputs, precision=lax.Precision.HIGHEST)
    pushed_imag = jnp.einsum("gpc,bsgc->bsgp", inject_imag, inputs, precision=lax.Precision.HIGHEST)
    state_real_part = carried[0].reshape(sequences, groups, entries)
    state_imaginary = carried[1].reshape(sequences, groups, entries)
    readings = []
    for position in range(positions):
        active_now = (active[:, position] > 0)[:, None, None]
        moved_real = (
            decay_real * state_real_part - decay_imag * state_imaginary + pushed_real[:, position]
        )
        moved_imag = (
            decay_real * state_imaginary + decay_imag * state_real_part + pushed_imag[:, position]
        )
        state_real_part = jnp.where(active_now, moved_real, state_real_part)
        state_imaginary = jnp.where(active_now, moved_imag, state_imaginary)
        readout_value = jnp.einsum(
            "sal,usl->usa", output_couple[0], state_real_part, precision=lax.Precision.HIGHEST
        ) - jnp.einsum(
            "sal,usl->usa", output_couple[1], state_imaginary, precision=lax.Precision.HIGHEST
        )
        readings.append(readout_value)
    readout = jnp.stack(readings, axis=1) + skip_now.reshape(groups, members) * inputs
    final = jnp.stack(
        [
            state_real_part.reshape(sequences, groups * entries),
            state_imaginary.reshape(sequences, groups * entries),
        ]
    )
    return (readout.reshape(sequences * positions, groups * members), final)


def widen_model(values):
    return lax.all_gather(values, "tp", axis=1, tiled=True)


def widen_branch(values):
    return lax.all_gather(values, "tp", axis=1, tiled=True)


def project(gathered, weight):
    return jnp.dot(
        gathered,
        lax.all_gather(weight, "dp", axis=0, tiled=True),
        preferred_element_type=jnp.float32,
    )


def shards(
    tokens,
    lengths,
    norm_gains,
    drive_proj,
    open_proj,
    glu_proj,
    merge_proj,
    exit_proj,
    decay_rate,
    turn_rate,
    group_step_width,
    state_in,
    state_out,
    skip_gain,
    carried_state,
):
    sequences, positions, local_width = tokens.shape
    row_count = sequences * positions
    model_width = local_width * lax.axis_size("tp")
    first_col = lax.axis_index("tp") * local_width
    active = (lax.broadcasted_iota(jnp.int32, (sequences, positions), 1) < lengths[:, None]).astype(
        jnp.int32
    )
    active_rows = active.reshape(row_count, 1).astype(jnp.float32)
    residual = tokens.reshape(row_count, local_width)
    states = []
    for layer_index in range(norm_gains.shape[0]):
        norm_gain = norm_gains[layer_index]
        own_values = residual.astype(jnp.float32)
        squared_sum = lax.psum(jnp.sum(own_values * own_values, axis=1), "tp")
        inverse_rms = lax.rsqrt(squared_sum / model_width + EPS)[:, None]
        own_gain = lax.dynamic_slice_in_dim(norm_gain, first_col, local_width, 0)
        gathered = widen_model((own_values * inverse_rms * own_gain).astype(jnp.bfloat16))
        drive = project(gathered, drive_proj[layer_index])
        gate_open = jax.nn.sigmoid(project(gathered, open_proj[layer_index]))
        readout, final = state_update(
            drive,
            active,
            decay_rate[layer_index],
            turn_rate[layer_index],
            group_step_width[layer_index],
            state_in[layer_index],
            state_out[layer_index],
            skip_gain[layer_index],
            carried_state[layer_index],
        )
        states.append(final)
        activated = jax.nn.gelu(readout).astype(jnp.bfloat16)
        gating = project(widen_branch(activated), glu_proj[layer_index])
        gated = (activated.astype(jnp.float32) * jax.nn.sigmoid(gating)).astype(jnp.bfloat16)
        merged = project(widen_branch(gated), merge_proj[layer_index])
        mixed = (gate_open * merged).astype(jnp.bfloat16)
        branch = project(widen_model(mixed), exit_proj[layer_index])
        residual = (residual.astype(jnp.float32) + active_rows * branch).astype(jnp.bfloat16)
    return (residual.reshape(sequences, positions, local_width), jnp.stack(states))


def fused_kernel(
    dims,
    tok, pack_own, unpack_own, keep, unpack, pack, gains, decay, inject, outmix, skip, carried,
    w_drive, w_open, w_glu, w_merge, w_exit,
    out_tok, out_state,
    v_drive, v_open, v_glu, v_merge, v_exit,
    row_send, row_recv, a_send, a_recv, c_send, c_recv,
    x_src, x_recv, y_src, y_recv, st_recv, st_new, nst_recv, fin_recv,
    inv_buf, gate_buf, act_buf,
    w_sem, row_ss, row_rs, a_ss, a_rs, c_ss, c_rs, x_ss, x_rs, y_ss, y_rs,
    st_ss, st_rs, n_ss, n_rs, f_ss, f_rs,
):
    layers, nd, nt, all_rows, model, lots = dims
    ratio = nt // nd
    rows = all_rows // lots
    chunk = rows // nd
    half = rows // 2
    f32, bf16 = jnp.float32, jnp.bfloat16
    d = lax.axis_index("dp")
    t = lax.axis_index("tp")
    home = t // ratio
    place = lax.rem(t, ratio)
    batch_own = carried.shape[2]
    batch = batch_own * nd
    own_ch = inject.shape[2] // 2
    width = c_send.shape[-1] // 2
    steps = unpack.shape[0] // batch

    loads = []
    for i, (src, dst) in enumerate(
        ((w_drive, v_drive), (w_open, v_open), (w_glu, v_glu), (w_merge, v_merge), (w_exit, v_exit))
    ):
        for l in range(layers):
            copy = pltpu.make_async_copy(src.at[l], dst.at[l], w_sem.at[i, l])
            copy.start()
            loads.append(copy)

    def weight(i, l):
        loads[i * layers + l].wait()

    barrier = pltpu.get_barrier_semaphore()
    total = nd * nt
    flat = t * nd + d

    def greet(i, carry):
        other = lax.rem(flat + i, total)
        pl.semaphore_signal(
            barrier, inc=1,
            device_id={"tp": other // nd, "dp": lax.rem(other, nd)},
            device_id_type=pl.DeviceIdType.MESH,
        )
        return carry

    lax.fori_loop(1, total, greet, 0)
    pl.semaphore_wait(barrier, total - 1)

    pending = []

    def send(src, dst, ss, rs, to_dp, to_tp, is_self):
        far = pltpu.make_async_remote_copy(
            src_ref=src, dst_ref=dst, send_sem=ss, recv_sem=rs,
            device_id={"tp": to_tp, "dp": to_dp}, device_id_type=pl.DeviceIdType.MESH,
        )
        if is_self is None:
            far.start()
        else:
            @pl.when(is_self)
            def _():
                pltpu.make_async_copy(src, dst, rs).start()

            @pl.when(jnp.logical_not(is_self))
            def _():
                far.start()

        pending.append((far, is_self))

    def arrive(dst, rs):
        pltpu.make_async_copy(dst, dst, rs).wait()

    def send_row(k, c):
        send(row_send.at[k, c], row_recv.at[k, d], row_ss.at[k, c], row_rs.at[k, d], c, t, d == c)

    def row_sum(k):
        acc = None
        for s in range(nd):
            arrive(row_recv.at[k, s], row_rs.at[k, s])
            v = row_recv[k, s].astype(f32)
            acc = v if acc is None else acc + v
        return acc

    def spread_x(k):
        slot = place * nd + d
        for j in range(nd):
            to = lax.rem(home + j, nd) * ratio + place
            send(
                x_src.at[k], x_recv.at[k, place, pl.ds(d * chunk, chunk)],
                x_ss.at[k, j], x_rs.at[k, slot], home, to, (d == home) if j == 0 else None,
            )

    def forward_x(k):
        for s in range(nd):
            piece = x_recv.at[k, place, pl.ds(s * chunk, chunk)]
            arrive(piece, x_rs.at[k, place * nd + s])
            for i in range(1, ratio):
                to = home * ratio + lax.rem(place + i, ratio)
                send(
                    piece, piece, x_ss.at[k, nd + s * (ratio - 1) + i - 1],
                    x_rs.at[k, place * nd + s], d, to, None,
                )

    def take_x(k):
        for i in range(1, ratio):
            p = lax.rem(place + i, ratio)
            for s in range(nd):
                arrive(x_recv.at[k, p, pl.ds(s * chunk, chunk)], x_rs.at[k, p * nd + s])

    def spread_y(k):
        slot = place * nd + d
        for j in range(nd):
            to = lax.rem(home + j, nd) * ratio + place
            send(
                y_src.at[k], y_recv.at[k, slot],
                y_ss.at[k, j], y_rs.at[k, slot], home, to, (d == home) if j == 0 else None,
            )

    def forward_y(k):
        for s in range(nd):
            slot = place * nd + s
            piece = y_recv.at[k, slot]
            arrive(piece, y_rs.at[k, slot])
            for i in range(1, ratio):
                to = home * ratio + lax.rem(place + i, ratio)
                send(
                    piece, piece, y_ss.at[k, nd + s * (ratio - 1) + i - 1],
                    y_rs.at[k, slot], d, to, None,
                )

    def take_y(k):
        for i in range(1, ratio):
            p = lax.rem(place + i, ratio)
            for s in range(nd):
                arrive(y_recv.at[k, p * nd + s], y_rs.at[k, p * nd + s])
        parts = []
        for p in range(ratio):
            for s in range(nd):
                v = y_recv[k, p * nd + s]
                parts.append(jnp.concatenate([v[:, :width], v[:, width:]], axis=0))
        return jnp.concatenate(parts, axis=1)

    def fold(v):
        return jnp.concatenate([v[:half], v[half:]], axis=1)

    every = range(lots)
    for h in every:
        for c in range(nd):
            top = h * rows + c * chunk
            part = jnp.dot(pack_own[top:top + chunk, :], tok[...], preferred_element_type=f32)
            row_send[h, c] = part.astype(bf16)
            send_row(h, c)
    for c in range(nd):
        send(
            carried.at[:, :, :, pl.ds(c * own_ch, own_ch)], st_recv.at[d],
            st_ss.at[c], st_rs.at[d], c, t, d == c,
        )
    cols = tok.shape[1]
    residual = []
    for h in every:
        residual.append(row_sum(h).astype(bf16))
        x_src[h] = residual[h]
        spread_x(h)
    for s in range(nd):
        arrive(st_recv.at[s], st_rs.at[s])
    for l in range(layers):
        first, second = 2 * l * lots, (2 * l + 1) * lots
        k_open = (1 + 3 * l) * lots
        k_merge, k_exit = k_open + lots, k_open + 2 * lots
        for h in every:
            forward_x(first + h)
        weight(0, l)
        normed = []
        for h in every:
            take_x(first + h)
            scaled, squares = [], None
            for p in range(ratio):
                raw = x_recv[first + h, p].astype(f32)
                sq = jnp.sum(raw * raw, axis=1, keepdims=True)
                squares = sq if squares is None else squares + sq
                scaled.append((raw * gains[l, p]).astype(bf16))
            normed.append(jnp.concatenate(scaled, axis=1))
            drive = jnp.dot(normed[h], v_drive[l], preferred_element_type=f32)
            high = squares.astype(bf16)
            low = (squares - high.astype(f32)).astype(bf16)
            lane = lax.broadcasted_iota(jnp.int32, (rows, width), 1)
            tail = jnp.where(
                lane == 0, high.astype(f32), jnp.where(lane == 1, low.astype(f32), 0.0)
            ).astype(bf16)
            k = l * lots + h
            for c in range(nd):
                a_send[k, c] = jnp.concatenate(
                    [drive[:, c * width:(c + 1) * width].astype(bf16), tail], axis=1
                )
                send(a_send.at[k, c], a_recv.at[k, d], a_ss.at[k, c], a_rs.at[k, d], c, t, d == c)
        weight(1, l)
        for h in every:
            for c in range(nd):
                part = jnp.dot(
                    normed[h][c * chunk:(c + 1) * chunk], v_open[l], preferred_element_type=f32
                )
                row_send[k_open + h, c] = part.astype(bf16)
                send_row(k_open + h, c)
        feeds = []
        for h in every:
            k = l * lots + h
            summed = None
            for s in range(nd):
                arrive(a_recv.at[k, s], a_rs.at[k, s])
                v = a_recv[k, s].astype(f32)
                summed = v if summed is None else summed + v
            full_sq = summed[:, width:width + 1] + summed[:, width + 1:width + 2]
            inverse = lax.rsqrt(full_sq / model + EPS)
            inv_buf[h * rows:(h + 1) * rows, :] = jnp.broadcast_to(inverse, (rows, 128))
            lane2 = lax.broadcasted_iota(jnp.int32, summed.shape, 1)
            feed = jnp.where(lane2 < width, summed * inverse, jnp.where(lane2 == width, 1.0, 0.0))
            feeds.append(feed.astype(bf16))
        feed = jnp.concatenate(feeds, axis=0)
        real = jnp.concatenate([st_recv[s, l, 0] for s in range(nd)], axis=0)
        imag = jnp.concatenate([st_recv[s, l, 1] for s in range(nd)], axis=0)
        dr, di = decay[l, 0], decay[l, 1]
        for step in range(steps):
            span = slice(step * batch, (step + 1) * batch)
            u = jnp.dot(unpack[span, :], feed, preferred_element_type=f32)
            live = u[:, width:width + 1] > 0.5
            push = jnp.dot(u.astype(bf16), inject[l], preferred_element_type=f32)
            moved_real = dr * real - di * imag + push[:, :own_ch]
            moved_imag = dr * imag + di * real + push[:, own_ch:]
            real = jnp.where(live, moved_real, real)
            imag = jnp.where(live, moved_imag, imag)
            both = jnp.concatenate([real, imag], axis=1).astype(bf16)
            read = jnp.dot(both, outmix[l], preferred_element_type=f32) + skip[l] * u
            act_buf[span, :] = jax.nn.gelu(read).astype(bf16)
        st_new[l, 0] = real
        st_new[l, 1] = imag
        activated = []
        for h in every:
            packed = jnp.dot(
                pack[h * rows:(h + 1) * rows, :], act_buf[...], preferred_element_type=f32
            ).astype(bf16)
            activated.append(fold(packed[:, :width]))
            y_src[first + h] = activated[h]
            spread_y(first + h)
        for h in every:
            mine = pl.ds(pl.multiple_of(h * rows + d * chunk, chunk), chunk)
            gate_buf[h] = jax.nn.sigmoid(row_sum(k_open + h) * inv_buf[mine, 0:1])
        weight(2, l)
        for h in every:
            forward_y(first + h)
        for h in every:
            wide = take_y(first + h)
            gating = jnp.dot(wide, v_glu[l], preferred_element_type=f32).astype(bf16)
            k = l * lots + h
            for c in range(nd):
                c_send[k, c] = fold(gating[:, c * width:(c + 1) * width])
                send(c_send.at[k, c], c_recv.at[k, d], c_ss.at[k, c], c_rs.at[k, d], c, t, d == c)
        for h in every:
            k = l * lots + h
            summed = None
            for s in range(nd):
                arrive(c_recv.at[k, s], c_rs.at[k, s])
                v = c_recv[k, s].astype(f32)
                summed = v if summed is None else summed + v
            gated = activated[h].astype(f32) * jax.nn.sigmoid(summed)
            y_src[second + h] = gated.astype(bf16)
            spread_y(second + h)
        weight(3, l)
        for h in every:
            forward_y(second + h)
        for h in every:
            wide = take_y(second + h)
            for c in range(nd):
                part = jnp.dot(
                    wide[c * chunk:(c + 1) * chunk], v_merge[l], preferred_element_type=f32
                )
                row_send[k_merge + h, c] = part.astype(bf16)
                send_row(k_merge + h, c)
        for h in every:
            x_src[second + h] = (gate_buf[h] * row_sum(k_merge + h)).astype(bf16)
            spread_x(second + h)
        for c in range(nd):
            send(
                st_new.at[l, :, pl.ds(c * batch_own, batch_own)], nst_recv.at[d, l],
                n_ss.at[l, c], n_rs.at[l, d], c, t, d == c,
            )
        weight(4, l)
        for h in every:
            forward_x(second + h)
        for h in every:
            take_x(second + h)
            for c in range(nd):
                part = None
                for p in range(ratio):
                    v = jnp.dot(
                        x_recv[second + h, p, c * chunk:(c + 1) * chunk],
                        v_exit[l, p * cols:(p + 1) * cols],
                        preferred_element_type=f32,
                    )
                    part = v if part is None else part + v
                row_send[k_exit + h, c] = part.astype(bf16)
                send_row(k_exit + h, c)
        for h in every:
            residual[h] = (residual[h].astype(f32) + row_sum(k_exit + h)).astype(bf16)
            k = (2 * l + 2) * lots + h
            x_src[k] = residual[h]
            if l + 1 < layers:
                spread_x(k)
            else:
                for c in range(nd):
                    send(
                        x_src.at[k], fin_recv.at[pl.ds(h * rows + d * chunk, chunk)],
                        f_ss.at[h, c], f_rs.at[h, d], c, t, d == c,
                    )
    for l in range(layers):
        for s in range(nd):
            arrive(nst_recv.at[s, l], n_rs.at[l, s])
            for part in range(2):
                out_state[l, part, :, s * own_ch:(s + 1) * own_ch] = nst_recv[s, l, part]
    for h in every:
        for s in range(nd):
            arrive(fin_recv.at[pl.ds(h * rows + s * chunk, chunk)], f_rs.at[h, s])
    spread = jnp.dot(unpack_own[...], fin_recv[...], preferred_element_type=f32)
    out_tok[...] = jnp.where(keep[...] > 0.5, spread, tok[...].astype(f32)).astype(bf16)
    for far, is_self in pending:
        if is_self is None:
            far.wait_send()
        else:
            pl.when(jnp.logical_not(is_self))(far.wait_send)


def fused_shards(
    tokens, lengths, norm_gains, drive_proj, open_proj, glu_proj, merge_proj, exit_proj,
    decay_rate, turn_rate, group_step_width, state_in, state_out, skip_gain, carried_state,
):
    f32, bf16 = jnp.float32, jnp.bfloat16
    nd, nt = lax.axis_size("dp"), lax.axis_size("tp")
    d, t = lax.axis_index("dp"), lax.axis_index("tp")
    layers = norm_gains.shape[0]
    own, steps, cols = tokens.shape
    batch = own * nd
    rows = 3 * batch
    model = cols * nt
    ratio = nt // nd
    groups_own = decay_rate.shape[1]
    few = groups_own // nd
    entries = decay_rate.shape[2]
    members = state_in.shape[-1]
    width = few * members
    own_ch = few * entries
    chunk = rows // nd

    everyone = lax.all_gather(lengths, "dp", axis=0, tiled=True)
    starts = jnp.cumsum(everyone) - everyone
    slot = jnp.arange(steps, dtype=jnp.int32)
    where_tb = jnp.where(
        slot[:, None] < everyone[None, :], starts[None, :] + slot[:, None], -1
    ).reshape(steps * batch)
    own_starts = lax.dynamic_slice_in_dim(starts, d * own, own, 0)
    where_own = jnp.where(
        slot[None, :] < lengths[:, None], own_starts[:, None] + slot[None, :], -1
    ).reshape(own * steps)
    index = jnp.arange(rows, dtype=jnp.int32)
    unpack = (where_tb[:, None] == index[None, :]).astype(bf16)
    pack = (index[:, None] == where_tb[None, :]).astype(bf16)
    unpack_own = (where_own[:, None] == index[None, :]).astype(bf16)
    pack_own = (index[:, None] == where_own[None, :]).astype(bf16)
    keep = (where_own >= 0).astype(f32)[:, None]
    gains = lax.dynamic_slice_in_dim(norm_gains, d * (model // nd), model // nd, 1).reshape(
        layers, ratio, 1, cols
    )

    def mine(v, axis):
        return lax.dynamic_slice_in_dim(v, d * few, few, axis)

    real_eig = -mine(decay_rate, 1)
    turn_now = mine(turn_rate, 1)
    step_len = mine(group_step_width, 1)[..., None]
    in_pair, out_pair = mine(state_in, 2), mine(state_out, 2)
    skip_now = mine(skip_gain.reshape(layers, groups_own, members), 1).reshape(layers, 1, width)
    magnitude = jnp.exp(step_len * real_eig)
    decay_real = magnitude * jnp.cos(step_len * turn_now)
    decay_imag = magnitude * jnp.sin(step_len * turn_now)
    divisor = real_eig * real_eig + turn_now * turn_now
    hold_real = ((decay_real - 1.0) * real_eig + decay_imag * turn_now) / divisor
    hold_imag = (decay_imag * real_eig - (decay_real - 1.0) * turn_now) / divisor
    inject_real = hold_real[..., None] * in_pair[:, 0] - hold_imag[..., None] * in_pair[:, 1]
    inject_imag = hold_real[..., None] * in_pair[:, 1] + hold_imag[..., None] * in_pair[:, 0]
    eye = jnp.eye(few, dtype=f32)
    both = jnp.stack([inject_real, inject_imag], axis=1)
    inject = (
        jnp.transpose(both, (0, 2, 4, 1, 3))[:, :, :, :, None, :]
        * eye[None, :, None, None, :, None]
    ).reshape(layers, width, 2 * own_ch)
    inject = jnp.pad(inject, ((0, 0), (0, width), (0, 0))).astype(bf16)
    signed = jnp.stack([out_pair[:, 0], -out_pair[:, 1]], axis=1)
    outmix = (
        jnp.transpose(signed, (0, 1, 2, 4, 3))[:, :, :, :, None, :]
        * eye[None, None, :, None, :, None]
    ).reshape(layers, 2 * own_ch, width)
    outmix = jnp.pad(outmix, ((0, 0), (0, 0), (0, width))).astype(bf16)
    skip = jnp.pad(skip_now, ((0, 0), (0, 0), (0, width)))
    decay = jnp.stack([decay_real, decay_imag], axis=1).reshape(layers, 2, 1, own_ch)

    lots = 2
    n_row = (1 + 3 * layers) * lots
    n_col = layers * lots
    n_all = 2 * layers * lots
    lot = rows // lots
    piece = chunk // lots
    half = lot // 2
    vm = pltpu.VMEM
    dma = pltpu.SemaphoreType.DMA
    weights = (drive_proj, open_proj, glu_proj, merge_proj, exit_proj)
    scratch = [vm(w.shape, bf16) for w in weights] + [
        vm((n_row, nd, piece, cols), bf16),
        vm((n_row, nd, piece, cols), bf16),
        vm((n_col, nd, lot, 2 * width), bf16),
        vm((n_col, nd, lot, 2 * width), bf16),
        vm((n_col, nd, half, 2 * width), bf16),
        vm((n_col, nd, half, 2 * width), bf16),
        vm((n_all + lots, piece, cols), bf16),
        vm((n_all, ratio, lot, cols), bf16),
        vm((n_all, half, 2 * width), bf16),
        vm((n_all, nt, half, 2 * width), bf16),
        vm((nd, layers, 2, own, own_ch), f32),
        vm((layers, 2, batch, own_ch), f32),
        vm((nd, layers, 2, own, own_ch), f32),
        vm((rows, cols), bf16),
        vm((rows, 128), f32),
        vm((lots, piece, cols), f32),
        vm((steps * batch, 2 * width), bf16),
        dma((5, layers)),
        dma((n_row, nd)), dma((n_row, nd)),
        dma((n_col, nd)), dma((n_col, nd)),
        dma((n_col, nd)), dma((n_col, nd)),
        dma((n_all, nd * ratio)), dma((n_all, nt)),
        dma((n_all, nd * ratio)), dma((n_all, nt)),
        dma((nd,)), dma((nd,)),
        dma((layers, nd)), dma((layers, nd)),
        dma((lots, nd)), dma((lots, nd)),
    ]
    inside = pl.BlockSpec(memory_space=pltpu.VMEM)
    outside = pl.BlockSpec(memory_space=pl.ANY)
    out_rows, out_state = pl.pallas_call(
        functools.partial(fused_kernel, (layers, nd, nt, rows, model, lots)),
        out_shape=(
            jax.ShapeDtypeStruct((own * steps, cols), bf16),
            jax.ShapeDtypeStruct(carried_state.shape, f32),
        ),
        in_specs=[inside] * 12 + [outside] * 5,
        out_specs=(inside, inside),
        scratch_shapes=scratch,
        compiler_params=pltpu.CompilerParams(
            collective_id=0, has_side_effects=True, vmem_limit_bytes=60 * 1024 * 1024
        ),
    )(
        tokens.reshape(own * steps, cols), pack_own, unpack_own, keep, unpack, pack,
        gains, decay, inject, outmix, skip, carried_state, *weights,
    )
    return out_rows.reshape(own, steps, cols), out_state


def solution(mesh):
    in_specs = (
        P("dp", None, "tp"),
        P("dp"),
        P(),
        P(None, "dp", "tp"),
        P(None, "dp", "tp"),
        P(None, "dp", "tp"),
        P(None, "dp", "tp"),
        P(None, "dp", "tp"),
        P(None, "tp", None),
        P(None, "tp", None),
        P(None, "tp"),
        P(None, None, "tp", None, None),
        P(None, None, "tp", None, None),
        P(None, "tp"),
        P(None, None, "dp", "tp"),
    )
    out_specs = (P("dp", None, "tp"), P(None, None, "dp", "tp"))
    ways, nd = mesh.shape["tp"], mesh.shape["dp"]

    def run(*args):
        groups = args[8].shape[1] // ways
        whole_groups = groups % nd == 0 and ways % nd == 0
        body = fused_shards if whole_groups else shards
        return jax.shard_map(body, mesh=mesh, in_specs=in_specs, out_specs=out_specs, check_vma=False)(*args)

    return run
```

```python
import functools
import jax
import jax.numpy as jnp
from jax import lax
from jax.experimental import pallas as pl
from jax.experimental.pallas import tpu as pltpu
from jax.sharding import PartitionSpec as P

EPS = 1e-05


def state_update(
    drive, active, current_rate, turn_now, size_now, in_pair, output_couple, skip_now, carried
):
    sequences, positions = active.shape
    groups, entries = current_rate.shape
    members = in_pair.shape[-1]
    real_eig = -current_rate
    step_len = size_now[:, None]
    magnitude = jnp.exp(step_len * real_eig)
    decay_real = magnitude * jnp.cos(step_len * turn_now)
    decay_imag = magnitude * jnp.sin(step_len * turn_now)
    divisor = real_eig * real_eig + turn_now * turn_now
    hold_real = ((decay_real - 1.0) * real_eig + decay_imag * turn_now) / divisor
    hold_imag = (decay_imag * real_eig - (decay_real - 1.0) * turn_now) / divisor
    inject_real = hold_real[..., None] * in_pair[0] - hold_imag[..., None] * in_pair[1]
    inject_imag = hold_real[..., None] * in_pair[1] + hold_imag[..., None] * in_pair[0]
    inputs = drive.reshape(sequences, positions, groups, members)
    pushed_real = jnp.einsum("gpc,bsgc->bsgp", inject_real, inputs, precision=lax.Precision.HIGHEST)
    pushed_imag = jnp.einsum("gpc,bsgc->bsgp", inject_imag, inputs, precision=lax.Precision.HIGHEST)
    state_real_part = carried[0].reshape(sequences, groups, entries)
    state_imaginary = carried[1].reshape(sequences, groups, entries)
    readings = []
    for position in range(positions):
        active_now = (active[:, position] > 0)[:, None, None]
        moved_real = (
            decay_real * state_real_part - decay_imag * state_imaginary + pushed_real[:, position]
        )
        moved_imag = (
            decay_real * state_imaginary + decay_imag * state_real_part + pushed_imag[:, position]
        )
        state_real_part = jnp.where(active_now, moved_real, state_real_part)
        state_imaginary = jnp.where(active_now, moved_imag, state_imaginary)
        readout_value = jnp.einsum(
            "sal,usl->usa", output_couple[0], state_real_part, precision=lax.Precision.HIGHEST
        ) - jnp.einsum(
            "sal,usl->usa", output_couple[1], state_imaginary, precision=lax.Precision.HIGHEST
        )
        readings.append(readout_value)
    readout = jnp.stack(readings, axis=1) + skip_now.reshape(groups, members) * inputs
    final = jnp.stack(
        [
            state_real_part.reshape(sequences, groups * entries),
            state_imaginary.reshape(sequences, groups * entries),
        ]
    )
    return (readout.reshape(sequences * positions, groups * members), final)


def widen_model(values):
    return lax.all_gather(values, "tp", axis=1, tiled=True)


def widen_branch(values):
    return lax.all_gather(values, "tp", axis=1, tiled=True)


def project(gathered, weight):
    return jnp.dot(
        gathered,
        lax.all_gather(weight, "dp", axis=0, tiled=True),
        preferred_element_type=jnp.float32,
    )


def shards(
    tokens,
    lengths,
    norm_gains,
    drive_proj,
    open_proj,
    glu_proj,
    merge_proj,
    exit_proj,
    decay_rate,
    turn_rate,
    group_step_width,
    state_in,
    state_out,
    skip_gain,
    carried_state,
):
    sequences, positions, local_width = tokens.shape
    row_count = sequences * positions
    model_width = local_width * lax.axis_size("tp")
    first_col = lax.axis_index("tp") * local_width
    active = (lax.broadcasted_iota(jnp.int32, (sequences, positions), 1) < lengths[:, None]).astype(
        jnp.int32
    )
    active_rows = active.reshape(row_count, 1).astype(jnp.float32)
    residual = tokens.reshape(row_count, local_width)
    states = []
    for layer_index in range(norm_gains.shape[0]):
        norm_gain = norm_gains[layer_index]
        own_values = residual.astype(jnp.float32)
        squared_sum = lax.psum(jnp.sum(own_values * own_values, axis=1), "tp")
        inverse_rms = lax.rsqrt(squared_sum / model_width + EPS)[:, None]
        own_gain = lax.dynamic_slice_in_dim(norm_gain, first_col, local_width, 0)
        gathered = widen_model((own_values * inverse_rms * own_gain).astype(jnp.bfloat16))
        drive = project(gathered, drive_proj[layer_index])
        gate_open = jax.nn.sigmoid(project(gathered, open_proj[layer_index]))
        readout, final = state_update(
            drive,
            active,
            decay_rate[layer_index],
            turn_rate[layer_index],
            group_step_width[layer_index],
            state_in[layer_index],
            state_out[layer_index],
            skip_gain[layer_index],
            carried_state[layer_index],
        )
        states.append(final)
        activated = jax.nn.gelu(readout).astype(jnp.bfloat16)
        gating = project(widen_branch(activated), glu_proj[layer_index])
        gated = (activated.astype(jnp.float32) * jax.nn.sigmoid(gating)).astype(jnp.bfloat16)
        merged = project(widen_branch(gated), merge_proj[layer_index])
        mixed = (gate_open * merged).astype(jnp.bfloat16)
        branch = project(widen_model(mixed), exit_proj[layer_index])
        residual = (residual.astype(jnp.float32) + active_rows * branch).astype(jnp.bfloat16)
    return (residual.reshape(sequences, positions, local_width), jnp.stack(states))


def fused_kernel(
    dims,
    tok, lens, gains, decay, inject, outmix, skip, carried,
    w_drive, w_open, w_glu, w_merge, w_exit,
    out_tok, out_state,
    v_drive, v_open, v_glu, v_merge, v_exit,
    row_send, row_recv, a_send, a_recv, c_send, c_recv,
    x_src, x_recv, y_src, y_recv, st_recv, st_new, nst_recv, fin_recv,
    inv_buf, gate_buf, act_buf, len_recv, pack_own, unpack,
    w_sem, row_ss, row_rs, a_ss, a_rs, c_ss, c_rs, x_ss, x_rs, y_ss, y_rs,
    st_ss, st_rs, n_ss, n_rs, f_ss, f_rs, l_ss, l_rs,
):
    layers, nd, nt, all_rows, model, lots = dims
    ratio = nt // nd
    rows = all_rows // lots
    chunk = rows // nd
    half = rows // 2
    f32, bf16 = jnp.float32, jnp.bfloat16
    d = lax.axis_index("dp")
    t = lax.axis_index("tp")
    home = t // ratio
    place = lax.rem(t, ratio)
    batch_own = carried.shape[2]
    batch = batch_own * nd
    own_ch = inject.shape[3] // 2
    width = c_send.shape[-1] // 2
    steps = tok.shape[0] // batch_own

    loads = []
    for i, (src, dst) in enumerate(
        ((w_drive, v_drive), (w_open, v_open), (w_glu, v_glu), (w_merge, v_merge), (w_exit, v_exit))
    ):
        for l in range(layers):
            copy = pltpu.make_async_copy(src.at[l], dst.at[l], w_sem.at[i, l])
            copy.start()
            loads.append(copy)

    def weight(i, l):
        loads[i * layers + l].wait()

    barrier = pltpu.get_barrier_semaphore()
    total = nd * nt
    flat = t * nd + d

    def greet(i, carry):
        other = lax.rem(flat + i, total)
        pl.semaphore_signal(
            barrier, inc=1,
            device_id={"tp": other // nd, "dp": lax.rem(other, nd)},
            device_id_type=pl.DeviceIdType.MESH,
        )
        return carry

    lax.fori_loop(1, total, greet, 0)
    pl.semaphore_wait(barrier, total - 1)

    pending = []

    def send(src, dst, ss, rs, to_dp, to_tp, is_self):
        far = pltpu.make_async_remote_copy(
            src_ref=src, dst_ref=dst, send_sem=ss, recv_sem=rs,
            device_id={"tp": to_tp, "dp": to_dp}, device_id_type=pl.DeviceIdType.MESH,
        )
        if is_self is None:
            far.start()
        else:
            @pl.when(is_self)
            def _():
                pltpu.make_async_copy(src, dst, rs).start()

            @pl.when(jnp.logical_not(is_self))
            def _():
                far.start()

        pending.append((far, is_self))

    def arrive(dst, rs):
        pltpu.make_async_copy(dst, dst, rs).wait()

    def send_row(k, c):
        send(row_send.at[k, c], row_recv.at[k, d], row_ss.at[k, c], row_rs.at[k, d], c, t, d == c)

    def row_sum(k):
        acc = None
        for s in range(nd):
            arrive(row_recv.at[k, s], row_rs.at[k, s])
            v = row_recv[k, s].astype(f32)
            acc = v if acc is None else acc + v
        return acc

    def spread_x(k):
        slot = place * nd + d
        for j in range(nd):
            to = lax.rem(home + j, nd) * ratio + place
            send(
                x_src.at[k], x_recv.at[k, place, pl.ds(d * chunk, chunk)],
                x_ss.at[k, j], x_rs.at[k, slot], home, to, (d == home) if j == 0 else None,
            )

    def forward_x(k):
        for s in range(nd):
            piece = x_recv.at[k, place, pl.ds(s * chunk, chunk)]
            arrive(piece, x_rs.at[k, place * nd + s])
            for i in range(1, ratio):
                to = home * ratio + lax.rem(place + i, ratio)
                send(
                    piece, piece, x_ss.at[k, nd + s * (ratio - 1) + i - 1],
                    x_rs.at[k, place * nd + s], d, to, None,
                )

    def take_x(k):
        for i in range(1, ratio):
            p = lax.rem(place + i, ratio)
            for s in range(nd):
                arrive(x_recv.at[k, p, pl.ds(s * chunk, chunk)], x_rs.at[k, p * nd + s])

    def spread_y(k):
        slot = place * nd + d
        for j in range(nd):
            to = lax.rem(home + j, nd) * ratio + place
            send(
                y_src.at[k], y_recv.at[k, slot],
                y_ss.at[k, j], y_rs.at[k, slot], home, to, (d == home) if j == 0 else None,
            )

    def forward_y(k):
        for s in range(nd):
            slot = place * nd + s
            piece = y_recv.at[k, slot]
            arrive(piece, y_rs.at[k, slot])
            for i in range(1, ratio):
                to = home * ratio + lax.rem(place + i, ratio)
                send(
                    piece, piece, y_ss.at[k, nd + s * (ratio - 1) + i - 1],
                    y_rs.at[k, slot], d, to, None,
                )

    def take_y(k):
        for i in range(1, ratio):
            p = lax.rem(place + i, ratio)
            for s in range(nd):
                arrive(y_recv.at[k, p * nd + s], y_rs.at[k, p * nd + s])
        parts = []
        for p in range(ratio):
            for s in range(nd):
                v = y_recv[k, p * nd + s]
                parts.append(jnp.concatenate([v[:, :width], v[:, width:]], axis=0))
        return jnp.concatenate(parts, axis=1)

    def fold(v):
        return jnp.concatenate([v[:half], v[half:]], axis=1)

    for c in range(nd):
        send(lens, len_recv.at[d], l_ss.at[c], l_rs.at[d], c, t, d == c)
    len_row = None
    for s in range(nd):
        arrive(len_recv.at[s], l_rs.at[s])
        len_row = len_recv[s] if len_row is None else len_row + len_recv[s]
    down = lax.broadcasted_iota(jnp.int32, (batch, batch), 0)
    along = lax.broadcasted_iota(jnp.int32, (batch, batch), 1)
    before = jnp.where(down < along, 1.0, 0.0).astype(bf16)
    start_row = jnp.dot(len_row.astype(bf16), before, preferred_element_type=f32)

    def upright(v):
        wide = jnp.broadcast_to(v[0:1], (batch, batch))
        return jnp.sum(jnp.where(down == along, wide, 0.0), axis=1, keepdims=True)

    len_col, start_col = upright(len_row), upright(start_row)
    count = lax.broadcasted_iota(jnp.int32, (batch, all_rows), 1).astype(f32)
    for step in range(steps):
        hit = jnp.logical_and(count == start_col + step, len_col > step)
        unpack[step * batch:(step + 1) * batch, :] = jnp.where(hit, 1.0, 0.0).astype(bf16)
    own_rows = tok.shape[0]
    local = lax.broadcasted_iota(jnp.int32, (batch, own_rows), 0) - d * batch_own
    item = lax.broadcasted_iota(jnp.int32, (batch, own_rows), 1)
    inside = jnp.logical_and(item >= local * steps, item < (local + 1) * steps)
    expand = jnp.where(inside, 1.0, 0.0)
    order = (lax.broadcasted_iota(jnp.int32, len_row.shape, 1) - d * batch_own).astype(f32)
    exact = functools.partial(
        jnp.dot, preferred_element_type=f32, precision=lax.Precision.HIGHEST
    )
    spot = exact(start_row - steps * order, expand)[0:1]
    spot = spot + lax.broadcasted_iota(jnp.int32, (1, own_rows), 1).astype(f32)
    end = exact(start_row + len_row, expand)[0:1]
    spot = jnp.where(spot < end, spot, -1.0)
    tall = lax.broadcasted_iota(jnp.int32, (all_rows, own_rows), 0).astype(f32)
    pack_own[...] = jnp.where(tall == spot, 1.0, 0.0).astype(bf16)

    def turned(a, b):
        return lax.dot_general(a, b, (((0,), (0,)), ((), ())), preferred_element_type=f32)

    every = range(lots)
    for h in every:
        for c in range(nd):
            top = h * rows + c * chunk
            part = jnp.dot(pack_own[top:top + chunk, :], tok[...], preferred_element_type=f32)
            row_send[h, c] = part.astype(bf16)
            send_row(h, c)
    for c in range(nd):
        send(
            carried.at[:, :, :, pl.ds(c * own_ch, own_ch)], st_recv.at[d],
            st_ss.at[c], st_rs.at[d], c, t, d == c,
        )
    cols = tok.shape[1]
    residual = []
    for h in every:
        residual.append(row_sum(h).astype(bf16))
        x_src[h] = residual[h]
        spread_x(h)
    for s in range(nd):
        arrive(st_recv.at[s], st_rs.at[s])
    for l in range(layers):
        first, second = 2 * l * lots, (2 * l + 1) * lots
        k_open = (1 + 3 * l) * lots
        k_merge, k_exit = k_open + lots, k_open + 2 * lots
        for h in every:
            forward_x(first + h)
        weight(0, l)
        normed = []
        for h in every:
            take_x(first + h)
            scaled, squares = [], None
            for p in range(ratio):
                raw = x_recv[first + h, p].astype(f32)
                sq = jnp.sum(raw * raw, axis=1, keepdims=True)
                squares = sq if squares is None else squares + sq
                scaled.append((raw * gains[l, d, p]).astype(bf16))
            normed.append(jnp.concatenate(scaled, axis=1))
            drive = jnp.dot(normed[h], v_drive[l], preferred_element_type=f32)
            high = squares.astype(bf16)
            low = (squares - high.astype(f32)).astype(bf16)
            lane = lax.broadcasted_iota(jnp.int32, (rows, width), 1)
            tail = jnp.where(
                lane == 0, high.astype(f32), jnp.where(lane == 1, low.astype(f32), 0.0)
            ).astype(bf16)
            k = l * lots + h
            for c in range(nd):
                a_send[k, c] = jnp.concatenate(
                    [drive[:, c * width:(c + 1) * width].astype(bf16), tail], axis=1
                )
                send(a_send.at[k, c], a_recv.at[k, d], a_ss.at[k, c], a_rs.at[k, d], c, t, d == c)
        weight(1, l)
        for h in every:
            for c in range(nd):
                part = jnp.dot(
                    normed[h][c * chunk:(c + 1) * chunk], v_open[l], preferred_element_type=f32
                )
                row_send[k_open + h, c] = part.astype(bf16)
                send_row(k_open + h, c)
        feeds = []
        for h in every:
            k = l * lots + h
            summed = None
            for s in range(nd):
                arrive(a_recv.at[k, s], a_rs.at[k, s])
                v = a_recv[k, s].astype(f32)
                summed = v if summed is None else summed + v
            full_sq = summed[:, width:width + 1] + summed[:, width + 1:width + 2]
            inverse = lax.rsqrt(full_sq / model + EPS)
            inv_buf[h * rows:(h + 1) * rows, :] = jnp.broadcast_to(inverse, (rows, 128))
            lane2 = lax.broadcasted_iota(jnp.int32, summed.shape, 1)
            feed = jnp.where(lane2 < width, summed * inverse, jnp.where(lane2 == width, 1.0, 0.0))
            feeds.append(feed.astype(bf16))
        feed = jnp.concatenate(feeds, axis=0)
        real = jnp.concatenate([st_recv[s, l, 0] for s in range(nd)], axis=0)
        imag = jnp.concatenate([st_recv[s, l, 1] for s in range(nd)], axis=0)
        dr, di = decay[l, 0, d], decay[l, 1, d]
        for step in range(steps):
            span = slice(step * batch, (step + 1) * batch)
            u = jnp.dot(unpack[span, :], feed, preferred_element_type=f32)
            live = u[:, width:width + 1] > 0.5
            push = jnp.dot(u.astype(bf16), inject[l, d], preferred_element_type=f32)
            moved_real = dr * real - di * imag + push[:, :own_ch]
            moved_imag = dr * imag + di * real + push[:, own_ch:]
            real = jnp.where(live, moved_real, real)
            imag = jnp.where(live, moved_imag, imag)
            both = jnp.concatenate([real, imag], axis=1).astype(bf16)
            read = jnp.dot(both, outmix[l, d], preferred_element_type=f32) + skip[l, d] * u
            act_buf[span, :] = jax.nn.gelu(read).astype(bf16)
        st_new[l, 0] = real
        st_new[l, 1] = imag
        packed_all = turned(unpack[...], act_buf[...]).astype(bf16)
        activated = []
        for h in every:
            packed = packed_all[h * rows:(h + 1) * rows]
            activated.append(fold(packed[:, :width]))
            y_src[first + h] = activated[h]
            spread_y(first + h)
        for h in every:
            mine = pl.ds(pl.multiple_of(h * rows + d * chunk, chunk), chunk)
            gate_buf[h] = jax.nn.sigmoid(row_sum(k_open + h) * inv_buf[mine, 0:1])
        weight(2, l)
        for h in every:
            forward_y(first + h)
        for h in every:
            wide = take_y(first + h)
            gating = jnp.dot(wide, v_glu[l], preferred_element_type=f32).astype(bf16)
            k = l * lots + h
            for c in range(nd):
                c_send[k, c] = fold(gating[:, c * width:(c + 1) * width])
                send(c_send.at[k, c], c_recv.at[k, d], c_ss.at[k, c], c_rs.at[k, d], c, t, d == c)
        for h in every:
            k = l * lots + h
            summed = None
            for s in range(nd):
                arrive(c_recv.at[k, s], c_rs.at[k, s])
                v = c_recv[k, s].astype(f32)
                summed = v if summed is None else summed + v
            gated = activated[h].astype(f32) * jax.nn.sigmoid(summed)
            y_src[second + h] = gated.astype(bf16)
            spread_y(second + h)
        weight(3, l)
        for h in every:
            forward_y(second + h)
        for h in every:
            wide = take_y(second + h)
            for c in range(nd):
                part = jnp.dot(
                    wide[c * chunk:(c + 1) * chunk], v_merge[l], preferred_element_type=f32
                )
                row_send[k_merge + h, c] = part.astype(bf16)
                send_row(k_merge + h, c)
        for h in every:
            x_src[second + h] = (gate_buf[h] * row_sum(k_merge + h)).astype(bf16)
            spread_x(second + h)
        for c in range(nd):
            send(
                st_new.at[l, :, pl.ds(c * batch_own, batch_own)], nst_recv.at[d, l],
                n_ss.at[l, c], n_rs.at[l, d], c, t, d == c,
            )
        weight(4, l)
        for h in every:
            forward_x(second + h)
        for h in every:
            take_x(second + h)
            for c in range(nd):
                part = None
                for p in range(ratio):
                    v = jnp.dot(
                        x_recv[second + h, p, c * chunk:(c + 1) * chunk],
                        v_exit[l, p * cols:(p + 1) * cols],
                        preferred_element_type=f32,
                    )
                    part = v if part is None else part + v
                row_send[k_exit + h, c] = part.astype(bf16)
                send_row(k_exit + h, c)
        for h in every:
            residual[h] = (residual[h].astype(f32) + row_sum(k_exit + h)).astype(bf16)
            k = (2 * l + 2) * lots + h
            x_src[k] = residual[h]
            if l + 1 < layers:
                spread_x(k)
            else:
                for c in range(nd):
                    send(
                        x_src.at[k], fin_recv.at[pl.ds(h * rows + d * chunk, chunk)],
                        f_ss.at[h, c], f_rs.at[h, d], c, t, d == c,
                    )
    for l in range(layers):
        for s in range(nd):
            arrive(nst_recv.at[s, l], n_rs.at[l, s])
            for part in range(2):
                out_state[l, part, :, s * own_ch:(s + 1) * own_ch] = nst_recv[s, l, part]
    for h in every:
        for s in range(nd):
            arrive(fin_recv.at[pl.ds(h * rows + s * chunk, chunk)], f_rs.at[h, s])
    spread = turned(pack_own[...], fin_recv[...])
    keep = turned(pack_own[...], jnp.ones((all_rows, 128), bf16))[:, 0:1]
    out_tok[...] = jnp.where(keep > 0.5, spread, tok[...].astype(f32)).astype(bf16)
    for far, is_self in pending:
        if is_self is None:
            far.wait_send()
        else:
            pl.when(jnp.logical_not(is_self))(far.wait_send)


def fused_shards(
    tokens, lengths, norm_gains, drive_proj, open_proj, glu_proj, merge_proj, exit_proj,
    decay_rate, turn_rate, group_step_width, state_in, state_out, skip_gain, carried_state,
):
    f32, bf16 = jnp.float32, jnp.bfloat16
    nd, nt = lax.axis_size("dp"), lax.axis_size("tp")
    d, t = lax.axis_index("dp"), lax.axis_index("tp")
    layers = norm_gains.shape[0]
    own, steps, cols = tokens.shape
    batch = own * nd
    rows = 3 * batch
    model = cols * nt
    ratio = nt // nd
    groups_own = decay_rate.shape[1]
    few = groups_own // nd
    entries = decay_rate.shape[2]
    members = state_in.shape[-1]
    width = few * members
    own_ch = few * entries
    chunk = rows // nd

    place = jnp.arange(batch, dtype=jnp.int32) // own
    lens = jnp.where(place == d, jnp.tile(lengths, nd), 0).astype(f32)
    lens = jnp.broadcast_to(lens[None, :], (8, batch))
    gains = norm_gains.reshape(layers, nd, ratio, 1, cols)

    real_eig = -decay_rate
    turn_now = turn_rate
    step_len = group_step_width[..., None]
    in_pair, out_pair = state_in, state_out
    skip_now = skip_gain.reshape(layers, nd, 1, width)
    magnitude = jnp.exp(step_len * real_eig)
    decay_real = magnitude * jnp.cos(step_len * turn_now)
    decay_imag = magnitude * jnp.sin(step_len * turn_now)
    divisor = real_eig * real_eig + turn_now * turn_now
    hold_real = ((decay_real - 1.0) * real_eig + decay_imag * turn_now) / divisor
    hold_imag = (decay_imag * real_eig - (decay_real - 1.0) * turn_now) / divisor
    inject_real = hold_real[..., None] * in_pair[:, 0] - hold_imag[..., None] * in_pair[:, 1]
    inject_imag = hold_real[..., None] * in_pair[:, 1] + hold_imag[..., None] * in_pair[:, 0]
    eye = jnp.eye(few, dtype=f32)
    both = jnp.stack([inject_real, inject_imag], axis=1).reshape(
        layers, 2, nd, few, entries, members
    )
    inject = (
        jnp.transpose(both, (0, 2, 3, 5, 1, 4))[:, :, :, :, :, None, :]
        * eye[None, None, :, None, None, :, None]
    ).reshape(layers, nd, width, 2 * own_ch)
    inject = jnp.pad(inject, ((0, 0), (0, 0), (0, width), (0, 0))).astype(bf16)
    signed = jnp.stack([out_pair[:, 0], -out_pair[:, 1]], axis=1).reshape(
        layers, 2, nd, few, members, entries
    )
    outmix = (
        jnp.transpose(signed, (0, 2, 1, 3, 5, 4))[:, :, :, :, :, None, :]
        * eye[None, None, None, :, None, :, None]
    ).reshape(layers, nd, 2 * own_ch, width)
    outmix = jnp.pad(outmix, ((0, 0), (0, 0), (0, 0), (0, width))).astype(bf16)
    skip = jnp.pad(skip_now, ((0, 0), (0, 0), (0, 0), (0, width)))
    decay = jnp.stack([decay_real, decay_imag], axis=1).reshape(layers, 2, nd, 1, own_ch)

    lots = 3
    n_row = (1 + 3 * layers) * lots
    n_col = layers * lots
    n_all = 2 * layers * lots
    lot = rows // lots
    piece = chunk // lots
    half = lot // 2
    vm = pltpu.VMEM
    dma = pltpu.SemaphoreType.DMA
    weights = (drive_proj, open_proj, glu_proj, merge_proj, exit_proj)
    scratch = [vm(w.shape, bf16) for w in weights] + [
        vm((n_row, nd, piece, cols), bf16),
        vm((n_row, nd, piece, cols), bf16),
        vm((n_col, nd, lot, 2 * width), bf16),
        vm((n_col, nd, lot, 2 * width), bf16),
        vm((n_col, nd, half, 2 * width), bf16),
        vm((n_col, nd, half, 2 * width), bf16),
        vm((n_all + lots, piece, cols), bf16),
        vm((n_all, ratio, lot, cols), bf16),
        vm((n_all, half, 2 * width), bf16),
        vm((n_all, nt, half, 2 * width), bf16),
        vm((nd, layers, 2, own, own_ch), f32),
        vm((layers, 2, batch, own_ch), f32),
        vm((nd, layers, 2, own, own_ch), f32),
        vm((rows, cols), bf16),
        vm((rows, 128), f32),
        vm((lots, piece, cols), f32),
        vm((steps * batch, 2 * width), bf16),
        vm((nd, 8, batch), f32),
        vm((rows, own * steps), bf16),
        vm((steps * batch, rows), bf16),
        dma((5, layers)),
        dma((n_row, nd)), dma((n_row, nd)),
        dma((n_col, nd)), dma((n_col, nd)),
        dma((n_col, nd)), dma((n_col, nd)),
        dma((n_all, nd * ratio)), dma((n_all, nt)),
        dma((n_all, nd * ratio)), dma((n_all, nt)),
        dma((nd,)), dma((nd,)),
        dma((layers, nd)), dma((layers, nd)),
        dma((lots, nd)), dma((lots, nd)),
        dma((nd,)), dma((nd,)),
    ]
    inside = pl.BlockSpec(memory_space=pltpu.VMEM)
    outside = pl.BlockSpec(memory_space=pl.ANY)
    out_rows, out_state = pl.pallas_call(
        functools.partial(fused_kernel, (layers, nd, nt, rows, model, lots)),
        out_shape=(
            jax.ShapeDtypeStruct((own * steps, cols), bf16),
            jax.ShapeDtypeStruct(carried_state.shape, f32),
        ),
        in_specs=[inside] * 8 + [outside] * 5,
        out_specs=(inside, inside),
        scratch_shapes=scratch,
        compiler_params=pltpu.CompilerParams(
            collective_id=0, has_side_effects=True, vmem_limit_bytes=60 * 1024 * 1024
        ),
    )(
        tokens.reshape(own * steps, cols), lens,
        gains, decay, inject, outmix, skip, carried_state, *weights,
    )
    return out_rows.reshape(own, steps, cols), out_state


def solution(mesh):
    in_specs = (
        P("dp", None, "tp"),
        P("dp"),
        P(),
        P(None, "dp", "tp"),
        P(None, "dp", "tp"),
        P(None, "dp", "tp"),
        P(None, "dp", "tp"),
        P(None, "dp", "tp"),
        P(None, "tp", None),
        P(None, "tp", None),
        P(None, "tp"),
        P(None, None, "tp", None, None),
        P(None, None, "tp", None, None),
        P(None, "tp"),
        P(None, None, "dp", "tp"),
    )
    out_specs = (P("dp", None, "tp"), P(None, None, "dp", "tp"))
    ways, nd = mesh.shape["tp"], mesh.shape["dp"]

    def run(*args):
        groups = args[8].shape[1] // ways
        whole_groups = groups % nd == 0 and ways % nd == 0
        body = fused_shards if whole_groups else shards
        return jax.shard_map(body, mesh=mesh, in_specs=in_specs, out_specs=out_specs, check_vma=False)(*args)

    return run
```
